512 devices in a mesh: grp: 2 (over y), sp: 64 (over z, core), tp: 4 (over x).
Axes of the slice: x: 4, y: 2, z: 32, core: 2. Of those that a mesh axis runs over, the one named last changes fastest.
The devices are a block of a 4x8x32 slice.
Arguments:
- tokens: bfloat16 [65536, 2048], P(('grp', 'sp')), parts along dimension 0, may hold values from -6 to 6
- gate_in: bfloat16 [2, 2048, 512], P(None, 'sp', 'tp'), may hold values from -0.125 to 0.125
- gate_conv: bfloat16 [2, 2048, 512], P(None, 'sp', 'tp'), may hold values from -0.125 to 0.125
- value_in: bfloat16 [2, 2048, 512], P(None, 'sp', 'tp'), may hold values from -0.125 to 0.125
- out_weight: bfloat16 [2, 512, 2048], P(None, None, 'sp'), may hold values from -0.25 to 0.25
- conv_taps: float32 [2, 3, 512], replicated, may hold values from -7 to 7
- pre_gain: float32 [2, 2048], replicated, may hold values from 0.1 to 1.9
- mix_gain: float32 [2, 512], replicated, may hold values from 0.1 to 1.9
- post_gain: float32 [2, 2048], replicated, may hold values from 0.1 to 1.9
Outputs:
- result: bfloat16 [65536, 2048], P(('grp', 'sp', 'tp')), parts along dimension 0
The draws below stay inside these ranges and needn't reach their ends.
There are 2 independent parts, one for each index of `grp`. The reference program is written for one: setup_inputs(seed, part) draws one part's arguments, and reference() takes and returns one part's arrays. A program takes and returns all parts, laid end to end along the dimension named above; an argument that names none is the same for every part. Nothing has to cross between parts.
All inputs are finite; a program needn't handle non-finite values.
Results may differ from the reference program's by a relative error of at most 0.011.
Values may be sent and summed in bfloat16 or wider, within the bound.
A program may use at most 64 MiB of HBM per device.

```python
import math
import jax
import jax.numpy as jnp
from jax import lax

D = 2048
S = 512
TAPS = 3
LAYERS = 2
TOKENS = 32768
TP_CH = 128


def draw_conv_taps(key, part):
    first_key, second_key = jax.random.split(jax.random.fold_in(key, 11))
    blocks = S // TP_CH
    orders = jax.vmap(lambda one_key: jax.random.permutation(one_key, blocks))(jax.random.split(first_key, LAYERS))
    ladder = 0.3 * jnp.power(10.0, orders.astype(jnp.float32) / max(blocks - 1, 1))
    raw_taps = jnp.clip(jax.random.normal(second_key, (LAYERS, TAPS, S), jnp.float32), -4.0, 4.0)
    scales = jnp.repeat(ladder, TP_CH, axis=1)
    return raw_taps * scales[:, None, :] / math.sqrt(TAPS)


def shard_levels(key, shape, shards, smallest, top_value):
    level = 1.0
    for dim, shards_of in shards:
        heights = jax.random.uniform(jax.random.fold_in(jax.random.fold_in(key, 6), dim), (shards_of,), jnp.float32, smallest / len(shards), top_value / len(shards))
        level = level * jnp.repeat(jnp.exp(heights), shape[dim] // shards_of).reshape((-1,) + (1,) * (len(shape) - 1 - dim))
    return level


def scatter_about(own_key, extent, scale, limit, cuts=(), dtype=jnp.bfloat16):
    loudness = shard_levels(own_key, extent, cuts, -0.22, 0.18) if cuts else 1.0
    array = jax.random.normal(own_key, extent, jnp.float32) * scale * loudness
    return jnp.minimum(jnp.maximum(array, -limit), limit).astype(dtype)


def setup_inputs(seed: int = 0, part: int = 0) -> dict:
    splits = jax.random.split(jax.random.key(seed), 10)
    own_keys = jax.random.split(jax.random.fold_in(splits[9], part), 10)
    return {
        "tokens": scatter_about(own_keys[0], (TOKENS, D), 1.0, 6.0, ((0, 64),)),
        "gate_in": scatter_about(splits[1], (LAYERS, D, S), D ** -0.5, 0.125, ((1, 64), (2, 4))),
        "gate_conv": scatter_about(splits[2], (LAYERS, D, S), D ** -0.5, 0.125, ((1, 64), (2, 4))),
        "value_in": scatter_about(splits[3], (LAYERS, D, S), D ** -0.5, 0.125, ((1, 64), (2, 4))),
        "out_weight": scatter_about(splits[4], (LAYERS, S, D), S ** -0.5, 0.25, ((2, 64),)),
        "conv_taps": draw_conv_taps(jax.random.fold_in(splits[9], 71), part),
        "pre_gain": jnp.clip(1.0 + 0.18 * jax.random.normal(splits[6], (LAYERS, D), jnp.float32), 0.1, 1.9),
        "mix_gain": jnp.clip(1.0 + 0.18 * jax.random.normal(splits[7], (LAYERS, S), jnp.float32), 0.1, 1.9),
        "post_gain": jnp.clip(1.0 + 0.18 * jax.random.normal(splits[8], (LAYERS, D), jnp.float32), 0.1, 1.9),
    }


EPS = 1e-06

def rms_norm(values, gain):
    return values * lax.rsqrt(lax.optimization_barrier(jnp.mean(values * values, axis=-1, keepdims=True)) + EPS) * gain

def stored(values):
    return lax.optimization_barrier(values.astype(jnp.bfloat16))

def reference(tokens, gate_in, gate_conv, value_in, out_weight, conv_taps, pre_gain, mix_gain, post_gain):
    stream = tokens.astype(jnp.float32)
    for layer_index in range(LAYERS):
        normed = stored(rms_norm(stream, pre_gain[layer_index]))
        outer = stored(jnp.dot(normed, gate_in[layer_index], preferred_element_type=jnp.float32))
        inner = stored(jnp.dot(normed, gate_conv[layer_index], preferred_element_type=jnp.float32))
        values = stored(jnp.dot(normed, value_in[layer_index], preferred_element_type=jnp.float32))
        gated = stored(inner.astype(jnp.float32) * values.astype(jnp.float32))
        padded = jnp.concatenate([jnp.zeros((TAPS - 1, S), jnp.bfloat16), gated], axis=0)
        filtered = jnp.zeros((TOKENS, S), jnp.float32)
        for tap_index in range(TAPS):
            filtered = filtered + conv_taps[layer_index, tap_index] * padded[tap_index:tap_index + TOKENS].astype(jnp.float32)
        mixed_raw = stored(outer.astype(jnp.float32) * filtered)
        mixed = stored(rms_norm(mixed_raw.astype(jnp.float32), mix_gain[layer_index]))
        branch = stored(jnp.dot(mixed, out_weight[layer_index], preferred_element_type=jnp.float32))
        stream = stream + rms_norm(branch.astype(jnp.float32), post_gain[layer_index])
    return stream.astype(jnp.bfloat16)
```

```python
import functools

import jax
import jax.numpy as jnp
from jax import lax
from jax.experimental import pallas as pl
from jax.experimental.pallas import tpu as pltpu
from jax.sharding import PartitionSpec as P

EPS = 1e-06
MESH = pl.DeviceIdType.MESH
F32 = jnp.float32
BF16 = jnp.bfloat16
LANES = 128
HALO = 16
BLOCK = 16


def block_kernel(
    sizes,
    tokens,
    gate_in,
    gate_conv,
    value_in,
    out_weight,
    conv_taps,
    pre_gain,
    mix_gain,
    post_gain,
    result,
    gates0,
    gates1,
    outs0,
    outs1,
    tok,
    normed,
    branch,
    stream,
    mixed_all,
    mixed_norm,
    mixed_own,
    mixed_rows,
    squares,
    load_sem,
    inj_send,
    inj_recv,
    cross_send,
    cross_recv,
    ring_send,
    ring_recv_a,
    ring_recv,
    halo_send,
    halo_recv,
    x_send,
    x_recv,
    a_send,
    a_recv,
):
    chips, tp_size, depth, rows, width, chans = sizes
    channels = tp_size * chans
    total = rows + HALO
    share = rows // tp_size
    sp = lax.axis_index("sp")
    tp = lax.axis_index("tp")
    z = sp // 2
    core = lax.rem(sp, 2)
    sgn = 1 - 2 * core
    minus = (9 * chips) // 16
    reaches = (chips - 1 - minus, minus)

    def chip(k):
        return lax.rem(z + k + 2 * chips, chips)

    partner = {"sp": z * 2 + 1 - core}
    ahead = {"sp": chip(sgn) * 2 + core}
    behind = {"sp": chip(-sgn) * 2 + core}
    follower = {"sp": lax.rem(sp + 1, 2 * chips)}
    leader = {"sp": lax.rem(sp + 2 * chips - 1, 2 * chips)}
    across = {"sp": jnp.where(core == 1, lax.rem(sp + 1, 2 * chips), lax.rem(sp + 2 * chips - 1, 2 * chips))}
    right = {"tp": lax.rem(tp + 1, tp_size)}
    left = {"tp": lax.rem(tp + tp_size - 1, tp_size)}

    barrier = pltpu.get_barrier_semaphore()
    peers = [partner, ahead, behind, across]
    peers += [{"tp": lax.rem(tp + j, tp_size)} for j in range(1, tp_size)]
    for peer in peers:
        pl.semaphore_signal(barrier, inc=1, device_id=peer, device_id_type=MESH)

    mine = pl.ds(pl.multiple_of(sp * depth, depth), depth)
    gates = (gates0, gates1)
    outs = (outs0, outs1)
    loads = []
    for layer in range(2):
        for j, weight in enumerate((gate_in, gate_conv, value_in)):
            copy = pltpu.make_async_copy(
                weight.at[layer], gates[layer].at[mine, pl.ds(j * chans, chans)], load_sem.at[3 * layer + j]
            )
            copy.start()
            loads.append(copy)
    for layer in range(2):
        copy = pltpu.make_async_copy(out_weight.at[layer], outs[layer].at[mine], load_sem.at[6 + layer])
        copy.start()
        loads.append(copy)
    load_tok = pltpu.make_async_copy(tokens, tok.at[pl.ds(HALO, rows)], load_sem.at[8])
    load_tok.start()

    buffers = (gates0, outs0, gates1, outs1)

    def one(zz, cc):
        return pl.ds(pl.multiple_of((zz * 2 + cc) * depth, depth), depth)

    def both(zz):
        return pl.ds(pl.multiple_of(zz * 2 * depth, 2 * depth), 2 * depth)

    def to_partner(s):
        ref = buffers[s].at[mine]
        return pltpu.make_async_remote_copy(
            src_ref=ref, dst_ref=ref, send_sem=inj_send.at[s], recv_sem=inj_recv.at[s],
            device_id=partner, device_id_type=MESH,
        )

    def from_partner(s):
        ref = buffers[s].at[one(z, 1 - core)]
        return pltpu.make_async_remote_copy(
            src_ref=ref, dst_ref=ref, send_sem=inj_send.at[s], recv_sem=inj_recv.at[s],
            device_id=partner, device_id_type=MESH,
        )

    def along(s, block, sem):
        ref = buffers[s].at[block]
        return pltpu.make_async_remote_copy(
            src_ref=ref, dst_ref=ref, send_sem=ring_send.at[s], recv_sem=sem,
            device_id=ahead, device_id_type=MESH,
        )

    def over(s, block):
        ref = buffers[s].at[block]
        return pltpu.make_async_remote_copy(
            src_ref=ref, dst_ref=ref, send_sem=cross_send.at[s], recv_sem=cross_recv.at[s],
            device_id=partner, device_id_type=MESH,
        )

    def relay_a(k, sub, reach):
        block = one(chip(-sgn * k), sub)
        along(0, block, ring_recv_a.at[sub, k]).wait_recv()

        @pl.when(k < reach)
        def _():
            along(0, block, ring_recv_a.at[sub, k + 1]).start()

        over(0, block).start()

    def relay(s, k, reach):
        block = both(chip(-sgn * k))
        along(s, block, ring_recv.at[s - 1, k]).wait_recv()

        @pl.when(k < reach)
        def _():
            along(s, block, ring_recv.at[s - 1, k + 1]).start()

        over(s, block).start()

    def halo_copy():
        return pltpu.make_async_remote_copy(
            src_ref=tokens.at[pl.ds(rows - HALO, HALO)], dst_ref=tok.at[pl.ds(0, HALO)],
            send_sem=halo_send, recv_sem=halo_recv, device_id=follower, device_id_type=MESH,
        )

    for copy in loads[:3]:
        copy.wait()
    pl.semaphore_wait(barrier, len(peers))
    along(0, mine, ring_recv_a.at[core, 1]).start()
    to_partner(0).start()
    for copy in loads[3:]:
        copy.wait()
    for s in (1, 2, 3):
        to_partner(s).start()
    from_partner(0).wait_recv()
    along(0, one(z, 1 - core), ring_recv_a.at[1 - core, 1]).start()
    for s in (1, 2, 3):
        from_partner(s).wait_recv()
        along(s, both(z), ring_recv.at[s - 1, 1]).start()

    @pl.when(sp < 2 * chips - 1)
    def _():
        halo_copy().start()

    @pl.when(sp == 0)
    def _():
        tok[pl.ds(0, HALO), :] = jnp.zeros((HALO, width), BF16)

    load_tok.wait()
    blocks = total // BLOCK

    def norm_block(b):
        at = pl.ds(pl.multiple_of(lax.rem(b + 1, blocks) * BLOCK, BLOCK), BLOCK)
        x = tok[at, :].astype(F32)
        scale = lax.rsqrt(jnp.sum(x * x, axis=-1, keepdims=True) / width + EPS)
        normed[at, :] = (x * scale * pre_gain[pl.ds(0, 1), :]).astype(BF16)

    def norm_some(k, count):
        for j in range(count):
            b = (k - 1) * count + j

            @pl.when((b == blocks - 1) & (sp > 0))
            def _():
                halo_copy().wait_recv()

            @pl.when(b < blocks)
            def _():
                norm_block(b)

    for cc in range(2):

        @pl.when(core == cc)
        def _(reach=reaches[cc]):
            def step(k, carry):
                relay_a(k, core, reach)
                relay_a(k, 1 - core, reach)
                for s in (1, 2, 3):
                    relay(s, k, reach)
                norm_some(k, -(-blocks // reach))
                return carry

            lax.fori_loop(1, reach + 1, step, 0)

    def arrived(s):
        for cc in range(2):

            @pl.when(core == cc)
            def _():
                over(s, pl.ds(0, reaches[1 - cc] * 2 * depth)).wait_recv()

    def mixing(layer):
        product = jnp.dot(normed[...], gates[layer][...], preferred_element_type=F32)
        outer = product[:, :chans].astype(BF16).astype(F32)
        inner = product[:, chans : 2 * chans].astype(BF16).astype(F32)
        values = product[:, 2 * chans :].astype(BF16).astype(F32)
        gated = (inner * values).astype(BF16).astype(F32)
        here = pl.ds(pl.multiple_of(tp * chans, chans), chans)
        taps = conv_taps[:, layer, here]
        filtered = (
            taps[0:1, :] * pltpu.roll(gated, 2, axis=0)
            + taps[1:2, :] * pltpu.roll(gated, 1, axis=0)
            + taps[2:3, :] * gated
        )
        return (outer * filtered).astype(BF16)

    def mix_norm(raw, layer):
        x = raw.astype(F32)
        scale = lax.rsqrt(jnp.sum(x * x, axis=-1, keepdims=True) / channels + EPS)
        return (x * scale * mix_gain[pl.ds(layer, 1), :]).astype(BF16)

    def lanes(j):
        return pl.ds(pl.multiple_of(lax.rem(j + tp_size, tp_size) * chans, chans), chans)

    arrived(0)
    mixed_all[:, lanes(tp)] = mixing(0)
    half = (total // BLOCK + 1) // 2 * BLOCK
    parts = (pl.ds(0, half), pl.ds(half, total - half))

    def swap(i, part, owner, to):
        ref = mixed_all.at[parts[part], lanes(owner)]
        return pltpu.make_async_remote_copy(
            src_ref=ref, dst_ref=ref, send_sem=x_send.at[i], recv_sem=x_recv.at[i], device_id=to, device_id_type=MESH
        )

    swap(0, 0, tp, right).start()
    swap(2, 1, tp, left).start()
    swap(1, 1, tp, right).start()
    swap(3, 0, tp, left).start()
    swap(0, 0, tp - 1, right).wait_recv()
    swap(4, 0, tp - 1, right).start()
    swap(2, 1, tp + 1, left).wait_recv()
    swap(5, 1, tp + 1, left).start()

    arrived(1)
    swap(1, 1, tp - 1, right).wait_recv()
    swap(3, 0, tp + 1, left).wait_recv()
    swap(4, 0, tp + 2, right).wait_recv()
    swap(5, 1, tp + 2, left).wait_recv()
    mixed_norm[...] = mix_norm(mixed_all[...], 0)
    tile = 2 * LANES
    tiles = width // tile

    def fold(x):
        return x[:, :LANES] + x[:, LANES:]

    squares[...] = jnp.zeros_like(squares)

    def project(n, carry):
        cols = pl.ds(pl.multiple_of(n * tile, tile), tile)
        out = lax.dot_general(
            mixed_norm[...], outs0[cols, :], (((1,), (1,)), ((), ())), preferred_element_type=F32
        ).astype(BF16)
        branch[:, cols] = out
        wide = out.astype(F32)
        squares[...] += fold(wide * wide)
        return carry

    lax.fori_loop(0, tiles, project, 0)
    group = 3

    def next_stream(i, carry):
        for j in range(group):
            b = i * group + j

            @pl.when(b < blocks)
            def _():
                at = pl.ds(pl.multiple_of(b * BLOCK, BLOCK), BLOCK)
                ss = jnp.sum(squares[at, :], axis=-1, keepdims=True)
                scale = lax.rsqrt(ss / width + EPS)
                new = tok[at, :].astype(F32) + branch[at, :].astype(F32) * scale * post_gain[pl.ds(0, 1), :]
                stream[at, :] = new
                scale = lax.rsqrt(jnp.sum(new * new, axis=-1, keepdims=True) / width + EPS)
                normed[at, :] = (new * scale * pre_gain[pl.ds(1, 1), :]).astype(BF16)

        return carry

    lax.fori_loop(0, -(-blocks // group), next_stream, 0)
    arrived(2)

    mixed_own[...] = mixing(1)[HALO:, :]

    def spread(j):
        to = lax.rem(tp + j, tp_size)
        return pltpu.make_async_remote_copy(
            src_ref=mixed_own.at[pl.ds(pl.multiple_of(to * share, share), share)],
            dst_ref=mixed_rows.at[:, lanes(tp)],
            send_sem=a_send.at[j], recv_sem=a_recv.at[j], device_id={"tp": to}, device_id_type=MESH,
        )

    def gathered(j):
        ref = mixed_rows.at[:, lanes(tp - j)]
        return pltpu.make_async_remote_copy(
            src_ref=ref, dst_ref=ref, send_sem=a_send.at[j], recv_sem=a_recv.at[j],
            device_id={"tp": lax.rem(tp + j, tp_size)}, device_id_type=MESH,
        )

    order = [2, 1, 3] if tp_size == 4 else list(range(1, tp_size))
    for j in order:
        spread(j).start()
    own_rows = pl.ds(pl.multiple_of(tp * share, share), share)
    mixed_rows[:, lanes(tp)] = mixed_own[own_rows, :]
    arrived(3)
    for j in order:
        gathered(j).wait_recv()
    mixed = mix_norm(mixed_rows[...], 1)
    sums = jnp.zeros((share, LANES), F32)
    for n in range(tiles):
        cols = pl.ds(n * tile, tile)
        out = lax.dot_general(
            mixed, outs1[cols, :], (((1,), (1,)), ((), ())), preferred_element_type=F32
        ).astype(BF16)
        branch[pl.ds(0, share), cols] = out
        wide = out.astype(F32)
        sums = sums + fold(wide * wide)
    squares[pl.ds(0, share), :] = sums

    def finish(b, carry):
        at = pl.ds(pl.multiple_of(b * BLOCK, BLOCK), BLOCK)
        scale = lax.rsqrt(jnp.sum(squares[at, :], axis=-1, keepdims=True) / width + EPS)
        held = pl.ds(pl.multiple_of(HALO + tp * share + b * BLOCK, BLOCK), BLOCK)
        result[at, :] = (
            stream[held, :] + branch[at, :].astype(F32) * scale * post_gain[pl.ds(1, 1), :]
        ).astype(BF16)
        return carry

    lax.fori_loop(0, share // BLOCK, finish, 0)

    @pl.when(sp < 2 * chips - 1)
    def _():
        halo_copy().wait_send()

    for j in order:
        spread(j).wait_send()
    for i, part in ((0, 0), (1, 1), (2, 1), (3, 0), (4, 0), (5, 1)):
        swap(i, part, tp, right).wait_send()
    for s in range(4):
        to_partner(s).wait_send()
        for cc in range(2):
            reach = reaches[cc]

            @pl.when(core == cc)
            def _(s=s, reach=reach):
                sent = pl.ds(0, reach * 2 * depth)
                along(s, sent, ring_recv.at[0, 0]).wait_send()
                over(s, sent).wait_send()


def solution(mesh):
    chips = mesh.shape["sp"] // 2
    tp_size = mesh.shape["tp"]

    def per_device(tokens, gate_in, gate_conv, value_in, out_weight, conv_taps, pre_gain, mix_gain, post_gain):
        rows, width = tokens.shape
        depth, chans = gate_in.shape[1:]
        channels = tp_size * chans
        total = rows + HALO
        share = rows // tp_size
        sizes = (chips, tp_size, depth, rows, width, chans)
        anywhere = pl.BlockSpec(memory_space=pl.ANY)
        inside = pl.BlockSpec(memory_space=pltpu.VMEM)
        dma = pltpu.SemaphoreType.DMA
        return pl.pallas_call(
            functools.partial(block_kernel, sizes),
            out_shape=jax.ShapeDtypeStruct((share, width), BF16),
            in_specs=[anywhere] * 5 + [inside] * 4,
            out_specs=inside,
            scratch_shapes=[
                pltpu.VMEM((width, 3 * chans), BF16),
                pltpu.VMEM((width, 3 * chans), BF16),
                pltpu.VMEM((width, channels), BF16),
                pltpu.VMEM((width, channels), BF16),
                pltpu.VMEM((total, width), BF16),
                pltpu.VMEM((total, width), BF16),
                pltpu.VMEM((total, width), BF16),
                pltpu.VMEM((total, width), F32),
                pltpu.VMEM((total, channels), BF16),
                pltpu.VMEM((total, channels), BF16),
                pltpu.VMEM((rows, chans), BF16),
                pltpu.VMEM((share, channels), BF16),
                pltpu.VMEM((total, LANES), F32),
                dma((9,)),
                dma((4,)),
                dma((4,)),
                dma((4,)),
                dma((4,)),
                dma((4,)),
                dma((2, chips)),
                dma((3, chips)),
                dma,
                dma,
                dma((6,)),
                dma((6,)),
                dma((tp_size,)),
                dma((tp_size,)),
            ],
            compiler_params=pltpu.CompilerParams(
                collective_id=0, has_side_effects=True, vmem_limit_bytes=56 * 2**20
            ),
            name="blocks",
        )(
            tokens,
            gate_in,
            gate_conv,
            value_in,
            jnp.swapaxes(out_weight, 1, 2),
            jnp.swapaxes(conv_taps, 0, 1),
            pre_gain,
            mix_gain,
            post_gain,
        )

    return jax.shard_map(
        per_device,
        mesh=mesh,
        in_specs=(
            P(("grp", "sp"), None),
            P(None, "sp", "tp"),
            P(None, "sp", "tp"),
            P(None, "sp", "tp"),
            P(None, None, "sp"),
            P(),
            P(),
            P(),
            P(),
        ),
        out_specs=P(("grp", "sp", "tp"), None),
        check_vma=False,
    )
```

```python
import functools

import jax
import jax.numpy as jnp
from jax import lax
from jax.experimental import pallas as pl
from jax.experimental.pallas import tpu as pltpu
from jax.sharding import PartitionSpec as P

EPS = 1e-06
MESH = pl.DeviceIdType.MESH
F32 = jnp.float32
BF16 = jnp.bfloat16
LANES = 128
HALO = 16
BLOCK = 16
LAG = 2


def block_kernel(
    sizes,
    tokens,
    gate_in,
    gate_conv,
    value_in,
    out_weight,
    conv_taps,
    pre_gain,
    mix_gain,
    post_gain,
    result,
    gates0,
    gates1,
    outs,
    tok,
    normed,
    branch,
    stream,
    mixed_all,
    mixed_norm,
    mixed_own,
    mixed_rows,
    squares,
    load_sem,
    inj_send,
    inj_recv,
    cross_send,
    cross_recv,
    ring_send,
    ring_recv,
    halo_send,
    halo_recv,
    x_send,
    x_recv,
    spread_send,
    spread_recv,
    a_send,
    a_recv,
):
    chips, tp_size, depth, rows, width, chans = sizes
    channels = tp_size * chans
    total = rows + HALO
    share = rows // tp_size
    sp = lax.axis_index("sp")
    tp = lax.axis_index("tp")
    z = sp // 2
    core = lax.rem(sp, 2)
    sgn = 1 - 2 * core
    minus = (9 * chips) // 16
    reaches = (chips - 1 - minus, minus)

    def chip(k):
        return lax.rem(z + k + 2 * chips, chips)

    partner = {"sp": z * 2 + 1 - core}
    ahead = {"sp": chip(sgn) * 2 + core}
    behind = {"sp": chip(-sgn) * 2 + core}
    follower = {"sp": lax.rem(sp + 1, 2 * chips)}
    leader = {"sp": lax.rem(sp + 2 * chips - 1, 2 * chips)}
    across = {"sp": jnp.where(core == 1, lax.rem(sp + 1, 2 * chips), lax.rem(sp + 2 * chips - 1, 2 * chips))}
    right = {"tp": lax.rem(tp + 1, tp_size)}
    left = {"tp": lax.rem(tp + tp_size - 1, tp_size)}

    barrier = pltpu.get_barrier_semaphore()
    peers = [partner, ahead, behind, across]
    peers += [{"tp": lax.rem(tp + j, tp_size)} for j in range(1, tp_size)]
    for peer in peers:
        pl.semaphore_signal(barrier, inc=1, device_id=peer, device_id_type=MESH)

    mine = pl.ds(pl.multiple_of(sp * depth, depth), depth)
    gates = (gates0, gates1)
    loads = []
    for layer in range(2):
        for j, weight in enumerate((gate_in, gate_conv, value_in)):
            copy = pltpu.make_async_copy(
                weight.at[layer], gates[layer].at[mine, pl.ds(j * chans, chans)], load_sem.at[3 * layer + j]
            )
            copy.start()
            loads.append(copy)
    for layer in range(2):
        for j in range(tp_size):
            copy = pltpu.make_async_copy(
                out_weight.at[layer, :, pl.ds(j * chans, chans)],
                outs.at[mine, pl.ds((2 * j + layer) * chans, chans)],
                load_sem.at[7 + layer * tp_size + j],
            )
            copy.start()
            loads.append(copy)
    load_tok = pltpu.make_async_copy(tokens, tok.at[pl.ds(HALO, rows)], load_sem.at[6])
    load_tok.start()

    buffers = (gates0, gates1, outs)

    def quarter(j):
        return pl.ds(pl.multiple_of(lax.rem(j + tp_size, tp_size) * 2 * chans, 2 * chans), 2 * chans)

    def part(s, block):
        return outs.at[block, quarter(tp)] if s == 2 else buffers[s].at[block]

    def one(zz, cc):
        return pl.ds(pl.multiple_of((zz * 2 + cc) * depth, depth), depth)

    def both(zz):
        return pl.ds(pl.multiple_of(zz * 2 * depth, 2 * depth), 2 * depth)

    def to_partner(s):
        ref = buffers[s].at[mine]
        return pltpu.make_async_remote_copy(
            src_ref=ref, dst_ref=ref, send_sem=inj_send.at[s], recv_sem=inj_recv.at[s],
            device_id=partner, device_id_type=MESH,
        )

    def from_partner(s):
        ref = buffers[s].at[one(z, 1 - core)]
        return pltpu.make_async_remote_copy(
            src_ref=ref, dst_ref=ref, send_sem=inj_send.at[s], recv_sem=inj_recv.at[s],
            device_id=partner, device_id_type=MESH,
        )

    def along(s, block, sem, to):
        ref = part(s, block)
        return pltpu.make_async_remote_copy(
            src_ref=ref, dst_ref=ref, send_sem=ring_send.at[s], recv_sem=sem, device_id=to, device_id_type=MESH
        )

    def cross(i, ref):
        return pltpu.make_async_remote_copy(
            src_ref=ref, dst_ref=ref, send_sem=cross_send.at[i], recv_sem=cross_recv.at[i],
            device_id=partner, device_id_type=MESH,
        )

    def launch(s, block, k, sub, reach):
        @pl.when(k < reach)
        def _():
            along(s, block, ring_recv.at[s, sub, k + 1], ahead).start()

    def relay(s, k, sub, reach):
        block = one(chip(-sgn * k), sub)
        along(s, block, ring_recv.at[s, sub, k], ahead).wait_recv()
        launch(s, block, k, sub, reach)
        cross(s, part(s, block)).start()

    def quarter_to(k, j):
        ref = outs.at[both(chip(-sgn * k)), quarter(tp)]
        return pltpu.make_async_remote_copy(
            src_ref=ref, dst_ref=ref, send_sem=spread_send, recv_sem=spread_recv.at[j - 1, k],
            device_id={"tp": lax.rem(tp + j, tp_size)}, device_id_type=MESH,
        )

    def quarters_in(k):
        for j in range(1, tp_size):
            ref = outs.at[both(chip(-sgn * k)), quarter(tp - j)]
            pltpu.make_async_remote_copy(
                src_ref=ref, dst_ref=ref, send_sem=spread_send, recv_sem=spread_recv.at[j - 1, k],
                device_id={"tp": lax.rem(tp + j, tp_size)}, device_id_type=MESH,
            ).wait_recv()
            cross(3, ref).start()

    def halo_copy():
        return pltpu.make_async_remote_copy(
            src_ref=tokens.at[pl.ds(rows - HALO, HALO)], dst_ref=tok.at[pl.ds(0, HALO)],
            send_sem=halo_send, recv_sem=halo_recv, device_id=follower, device_id_type=MESH,
        )

    for copy in loads[:3]:
        copy.wait()
    pl.semaphore_wait(barrier, len(peers))
    reach_here = jnp.where(core == 1, reaches[1], reaches[0])
    launch(0, mine, 0, core, reach_here)
    to_partner(0).start()
    for copy in loads[3:]:
        copy.wait()
    for s in (2, 1):
        launch(s, mine, 0, core, reach_here)
        to_partner(s).start()
    for s in (0, 2, 1):
        from_partner(s).wait_recv()
        launch(s, one(z, 1 - core), 0, 1 - core, reach_here)

    @pl.when(sp < 2 * chips - 1)
    def _():
        halo_copy().start()

    @pl.when(sp == 0)
    def _():
        tok[pl.ds(0, HALO), :] = jnp.zeros((HALO, width), BF16)

    load_tok.wait()
    blocks = total // BLOCK

    def norm_block(b):
        at = pl.ds(pl.multiple_of(lax.rem(b + 1, blocks) * BLOCK, BLOCK), BLOCK)
        x = tok[at, :].astype(F32)
        scale = lax.rsqrt(jnp.sum(x * x, axis=-1, keepdims=True) / width + EPS)
        normed[at, :] = (x * scale * pre_gain[pl.ds(0, 1), :]).astype(BF16)

    def norm_some(k, count):
        for j in range(count):
            b = (k - 1) * count + j

            @pl.when((b == blocks - 1) & (sp > 0))
            def _():
                halo_copy().wait_recv()

            @pl.when(b < blocks)
            def _():
                norm_block(b)

    for cc in range(2):

        @pl.when(core == cc)
        def _(reach=reaches[cc]):
            def step(k, carry):
                for s in (0, 2, 1):
                    relay(s, k, core, reach)
                    relay(s, k, 1 - core, reach)
                    if s == 2:
                        for j in range(1, tp_size):
                            quarter_to(k, j).start()
                norm_some(k, -(-blocks // reach))

                @pl.when(k > LAG)
                def _():
                    quarters_in(k - LAG)

                return carry

            lax.fori_loop(1, reach + 1, step, 0)

    def covering(i, reach):
        held = pl.ds(0, reach * 2 * depth)
        if i < 2:
            return buffers[i].at[held]
        return outs.at[held, pl.ds(0, 2 * chans * (1 if i == 2 else tp_size - 1))]

    def arrived(i):
        for cc in range(2):

            @pl.when(core == cc)
            def _():
                cross(i, covering(i, reaches[1 - cc])).wait_recv()

    def mixing(layer):
        product = jnp.dot(normed[...], gates[layer][...], preferred_element_type=F32)
        outer = product[:, :chans].astype(BF16).astype(F32)
        inner = product[:, chans : 2 * chans].astype(BF16).astype(F32)
        values = product[:, 2 * chans :].astype(BF16).astype(F32)
        gated = (inner * values).astype(BF16).astype(F32)
        here = pl.ds(pl.multiple_of(tp * chans, chans), chans)
        taps = conv_taps[:, layer, here]
        filtered = (
            taps[0:1, :] * pltpu.roll(gated, 2, axis=0)
            + taps[1:2, :] * pltpu.roll(gated, 1, axis=0)
            + taps[2:3, :] * gated
        )
        return (outer * filtered).astype(BF16)

    def mix_norm(raw, layer):
        x = raw.astype(F32)
        scale = lax.rsqrt(jnp.sum(x * x, axis=-1, keepdims=True) / channels + EPS)
        return (x * scale * mix_gain[pl.ds(layer, 1), :]).astype(BF16)

    def lanes(j):
        return pl.ds(pl.multiple_of(lax.rem(j + tp_size, tp_size) * chans, chans), chans)

    arrived(0)
    mixed_all[:, lanes(tp)] = mixing(0)
    half = (total // BLOCK + 1) // 2 * BLOCK
    parts = (pl.ds(0, half), pl.ds(half, total - half))

    def swap(i, part, owner, to):
        ref = mixed_all.at[parts[part], lanes(owner)]
        return pltpu.make_async_remote_copy(
            src_ref=ref, dst_ref=ref, send_sem=x_send.at[i], recv_sem=x_recv.at[i], device_id=to, device_id_type=MESH
        )

    swap(0, 0, tp, right).start()
    swap(2, 1, tp, left).start()
    swap(1, 1, tp, right).start()
    swap(3, 0, tp, left).start()
    swap(0, 0, tp - 1, right).wait_recv()
    swap(4, 0, tp - 1, right).start()
    swap(2, 1, tp + 1, left).wait_recv()
    swap(5, 1, tp + 1, left).start()

    for lag in reversed(range(LAG)):
        quarters_in(reach_here - lag)
    arrived(2)
    arrived(3)
    swap(1, 1, tp - 1, right).wait_recv()
    swap(3, 0, tp + 1, left).wait_recv()
    swap(4, 0, tp + 2, right).wait_recv()
    swap(5, 1, tp + 2, left).wait_recv()
    mixed_norm[...] = mix_norm(mixed_all[...], 0)
    tile = 2 * LANES
    tiles = width // tile

    def weights(cols, layer):
        return jnp.concatenate(
            [outs[cols, pl.ds((2 * j + layer) * chans, chans)] for j in range(tp_size)], axis=1
        )

    def fold(x):
        return x[:, :LANES] + x[:, LANES:]

    squares[...] = jnp.zeros_like(squares)

    def project(n, carry):
        cols = pl.ds(pl.multiple_of(n * tile, tile), tile)
        out = lax.dot_general(
            mixed_norm[...], weights(cols, 0), (((1,), (1,)), ((), ())), preferred_element_type=F32
        ).astype(BF16)
        branch[:, cols] = out
        wide = out.astype(F32)
        squares[...] += fold(wide * wide)
        return carry

    lax.fori_loop(0, tiles, project, 0)
    group = 3

    def next_stream(i, carry):
        for j in range(group):
            b = i * group + j

            @pl.when(b < blocks)
            def _():
                at = pl.ds(pl.multiple_of(b * BLOCK, BLOCK), BLOCK)
                ss = jnp.sum(squares[at, :], axis=-1, keepdims=True)
                scale = lax.rsqrt(ss / width + EPS)
                new = tok[at, :].astype(F32) + branch[at, :].astype(F32) * scale * post_gain[pl.ds(0, 1), :]
                stream[at, :] = new
                scale = lax.rsqrt(jnp.sum(new * new, axis=-1, keepdims=True) / width + EPS)
                normed[at, :] = (new * scale * pre_gain[pl.ds(1, 1), :]).astype(BF16)

        return carry

    lax.fori_loop(0, -(-blocks // group), next_stream, 0)
    arrived(1)

    mixed_own[...] = mixing(1)[HALO:, :]

    def spread(j):
        to = lax.rem(tp + j, tp_size)
        return pltpu.make_async_remote_copy(
            src_ref=mixed_own.at[pl.ds(pl.multiple_of(to * share, share), share)],
            dst_ref=mixed_rows.at[:, lanes(tp)],
            send_sem=a_send.at[j], recv_sem=a_recv.at[j], device_id={"tp": to}, device_id_type=MESH,
        )

    def gathered(j):
        ref = mixed_rows.at[:, lanes(tp - j)]
        return pltpu.make_async_remote_copy(
            src_ref=ref, dst_ref=ref, send_sem=a_send.at[j], recv_sem=a_recv.at[j],
            device_id={"tp": lax.rem(tp + j, tp_size)}, device_id_type=MESH,
        )

    order = [2, 1, 3] if tp_size == 4 else list(range(1, tp_size))
    for j in order:
        spread(j).start()
    own_rows = pl.ds(pl.multiple_of(tp * share, share), share)
    mixed_rows[:, lanes(tp)] = mixed_own[own_rows, :]
    for j in order:
        gathered(j).wait_recv()
    mixed = mix_norm(mixed_rows[...], 1)
    sums = jnp.zeros((share, LANES), F32)
    for n in range(tiles):
        cols = pl.ds(n * tile, tile)
        out = lax.dot_general(
            mixed, weights(cols, 1), (((1,), (1,)), ((), ())), preferred_element_type=F32
        ).astype(BF16)
        branch[pl.ds(0, share), cols] = out
        wide = out.astype(F32)
        sums = sums + fold(wide * wide)
    squares[pl.ds(0, share), :] = sums

    def finish(b, carry):
        at = pl.ds(pl.multiple_of(b * BLOCK, BLOCK), BLOCK)
        scale = lax.rsqrt(jnp.sum(squares[at, :], axis=-1, keepdims=True) / width + EPS)
        held = pl.ds(pl.multiple_of(HALO + tp * share + b * BLOCK, BLOCK), BLOCK)
        result[at, :] = (
            stream[held, :] + branch[at, :].astype(F32) * scale * post_gain[pl.ds(1, 1), :]
        ).astype(BF16)
        return carry

    lax.fori_loop(0, share // BLOCK, finish, 0)

    @pl.when(sp < 2 * chips - 1)
    def _():
        halo_copy().wait_send()

    for j in order:
        spread(j).wait_send()
    for i, part in ((0, 0), (1, 1), (2, 1), (3, 0), (4, 0), (5, 1)):
        swap(i, part, tp, right).wait_send()
    for s in range(3):
        to_partner(s).wait_send()
    for cc in range(2):

        @pl.when(core == cc)
        def _(reach=reaches[cc]):
            for i in range(4):
                cross(i, covering(i, reach)).wait_send()
            for i in range(3):
                along_all = pltpu.make_async_remote_copy(
                    src_ref=covering(i, reach), dst_ref=covering(i, reach), send_sem=ring_send.at[i],
                    recv_sem=ring_recv.at[0, 0, 0], device_id=ahead, device_id_type=MESH,
                )
                along_all.wait_send()
            pltpu.make_async_remote_copy(
                src_ref=covering(3, reach), dst_ref=covering(3, reach), send_sem=spread_send,
                recv_sem=ring_recv.at[0, 0, 0], device_id=right, device_id_type=MESH,
            ).wait_send()


def solution(mesh):
    chips = mesh.shape["sp"] // 2
    tp_size = mesh.shape["tp"]

    def per_device(tokens, gate_in, gate_conv, value_in, out_weight, conv_taps, pre_gain, mix_gain, post_gain):
        rows, width = tokens.shape
        depth, chans = gate_in.shape[1:]
        channels = tp_size * chans
        total = rows + HALO
        share = rows // tp_size
        sizes = (chips, tp_size, depth, rows, width, chans)
        anywhere = pl.BlockSpec(memory_space=pl.ANY)
        inside = pl.BlockSpec(memory_space=pltpu.VMEM)
        dma = pltpu.SemaphoreType.DMA
        return pl.pallas_call(
            functools.partial(block_kernel, sizes),
            out_shape=jax.ShapeDtypeStruct((share, width), BF16),
            in_specs=[anywhere] * 5 + [inside] * 4,
            out_specs=inside,
            scratch_shapes=[
                pltpu.VMEM((width, 3 * chans), BF16),
                pltpu.VMEM((width, 3 * chans), BF16),
                pltpu.VMEM((width, 2 * channels), BF16),
                pltpu.VMEM((total, width), BF16),
                pltpu.VMEM((total, width), BF16),
                pltpu.VMEM((total, width), BF16),
                pltpu.VMEM((total, width), F32),
                pltpu.VMEM((total, channels), BF16),
                pltpu.VMEM((total, channels), BF16),
                pltpu.VMEM((rows, chans), BF16),
                pltpu.VMEM((share, channels), BF16),
                pltpu.VMEM((total, LANES), F32),
                dma((7 + 2 * tp_size,)),
                dma((4,)),
                dma((4,)),
                dma((4,)),
                dma((4,)),
                dma((4,)),
                dma((3, 2, chips)),
                dma,
                dma,
                dma((6,)),
                dma((6,)),
                dma,
                dma((tp_size - 1, chips)),
                dma((tp_size,)),
                dma((tp_size,)),
            ],
            compiler_params=pltpu.CompilerParams(
                collective_id=0, has_side_effects=True, vmem_limit_bytes=56 * 2**20
            ),
            name="blocks",
        )(
            tokens,
            gate_in,
            gate_conv,
            value_in,
            jnp.swapaxes(out_weight, 1, 2),
            jnp.swapaxes(conv_taps, 0, 1),
            pre_gain,
            mix_gain,
            post_gain,
        )

    return jax.shard_map(
        per_device,
        mesh=mesh,
        in_specs=(
            P(("grp", "sp"), None),
            P(None, "sp", "tp"),
            P(None, "sp", "tp"),
            P(None, "sp", "tp"),
            P(None, None, "sp"),
            P(),
            P(),
            P(),
            P(),
        ),
        out_specs=P(("grp", "sp", "tp"), None),
        check_vma=False,
    )
```

```python
import functools

import jax
import jax.numpy as jnp
from jax import lax
from jax.experimental import pallas as pl
from jax.experimental.pallas import tpu as pltpu
from jax.sharding import PartitionSpec as P

EPS = 1e-06
MESH = pl.DeviceIdType.MESH
F32 = jnp.float32
BF16 = jnp.bfloat16
LANES = 128
HALO = 16
BLOCK = 16
LAG = 2


def block_kernel(
    sizes,
    tokens,
    gate_in,
    gate_conv,
    value_in,
    out_weight,
    conv_taps,
    pre_gain,
    mix_gain,
    post_gain,
    result,
    gates0,
    gates1,
    outs,
    tok,
    normed,
    branch,
    stream,
    mixed_all,
    mixed_norm,
    mixed_own,
    mixed_rows,
    squares,
    load_sem,
    inj_send,
    inj_recv,
    cross_send,
    cross_recv,
    ring_send,
    ring_recv,
    halo_send,
    halo_recv,
    x_send,
    x_recv,
    spread_send,
    spread_recv,
    a_send,
    a_recv,
):
    chips, tp_size, depth, rows, width, chans = sizes
    channels = tp_size * chans
    total = rows + HALO
    share = rows // tp_size
    sp = lax.axis_index("sp")
    tp = lax.axis_index("tp")
    z = sp // 2
    core = lax.rem(sp, 2)
    sgn = 1 - 2 * core
    minus = (9 * chips) // 16
    reaches = (chips - 1 - minus, minus)

    def chip(k):
        return lax.rem(z + k + 2 * chips, chips)

    partner = {"sp": z * 2 + 1 - core}
    ahead = {"sp": chip(sgn) * 2 + core}
    behind = {"sp": chip(-sgn) * 2 + core}
    follower = {"sp": lax.rem(sp + 1, 2 * chips)}
    leader = {"sp": lax.rem(sp + 2 * chips - 1, 2 * chips)}
    across = {"sp": jnp.where(core == 1, lax.rem(sp + 1, 2 * chips), lax.rem(sp + 2 * chips - 1, 2 * chips))}
    right = {"tp": lax.rem(tp + 1, tp_size)}
    left = {"tp": lax.rem(tp + tp_size - 1, tp_size)}

    barrier = pltpu.get_barrier_semaphore()
    peers = [partner, ahead, behind, across]
    peers += [{"tp": lax.rem(tp + j, tp_size)} for j in range(1, tp_size)]
    for peer in peers:
        pl.semaphore_signal(barrier, inc=1, device_id=peer, device_id_type=MESH)

    mine = pl.ds(pl.multiple_of(sp * depth, depth), depth)
    gates = (gates0, gates1)
    loads = []
    for layer in range(2):
        for j, weight in enumerate((gate_in, gate_conv, value_in)):
            copy = pltpu.make_async_copy(
                weight.at[layer], gates[layer].at[mine, pl.ds(j * chans, chans)], load_sem.at[3 * layer + j]
            )
            copy.start()
            loads.append(copy)
    for layer in range(2):
        for j in range(tp_size):
            copy = pltpu.make_async_copy(
                out_weight.at[layer, :, pl.ds(j * chans, chans)],
                outs.at[mine, pl.ds((2 * j + layer) * chans, chans)],
                load_sem.at[7 + layer * tp_size + j],
            )
            copy.start()
            loads.append(copy)
    load_tok = pltpu.make_async_copy(tokens, tok.at[pl.ds(HALO, rows)], load_sem.at[6])
    load_tok.start()

    buffers = (gates0, gates1, outs)

    def quarter(j):
        return pl.ds(pl.multiple_of(lax.rem(j + tp_size, tp_size) * 2 * chans, 2 * chans), 2 * chans)

    def part(s, block):
        return outs.at[block, quarter(tp)] if s == 2 else buffers[s].at[block]

    def one(zz, cc):
        return pl.ds(pl.multiple_of((zz * 2 + cc) * depth, depth), depth)

    def both(zz):
        return pl.ds(pl.multiple_of(zz * 2 * depth, 2 * depth), 2 * depth)

    def to_partner(s):
        ref = buffers[s].at[mine]
        return pltpu.make_async_remote_copy(
            src_ref=ref, dst_ref=ref, send_sem=inj_send.at[s], recv_sem=inj_recv.at[s],
            device_id=partner, device_id_type=MESH,
        )

    def from_partner(s):
        ref = buffers[s].at[one(z, 1 - core)]
        return pltpu.make_async_remote_copy(
            src_ref=ref, dst_ref=ref, send_sem=inj_send.at[s], recv_sem=inj_recv.at[s],
            device_id=partner, device_id_type=MESH,
        )

    def along(s, block, sem, to):
        ref = part(s, block)
        return pltpu.make_async_remote_copy(
            src_ref=ref, dst_ref=ref, send_sem=ring_send.at[s], recv_sem=sem, device_id=to, device_id_type=MESH
        )

    def cross(i, ref):
        return pltpu.make_async_remote_copy(
            src_ref=ref, dst_ref=ref, send_sem=cross_send.at[i], recv_sem=cross_recv.at[i],
            device_id=partner, device_id_type=MESH,
        )

    def launch(s, block, k, sub, reach):
        @pl.when(k < reach)
        def _():
            along(s, block, ring_recv.at[s, sub, k + 1], ahead).start()

    def relay(s, k, sub, reach):
        block = one(chip(-sgn * k), sub)
        along(s, block, ring_recv.at[s, sub, k], ahead).wait_recv()
        launch(s, block, k, sub, reach)
        cross(s, part(s, block)).start()

    def quarter_to(k, j):
        ref = outs.at[both(chip(-sgn * k)), quarter(tp)]
        return pltpu.make_async_remote_copy(
            src_ref=ref, dst_ref=ref, send_sem=spread_send, recv_sem=spread_recv.at[j - 1, k],
            device_id={"tp": lax.rem(tp + j, tp_size)}, device_id_type=MESH,
        )

    def quarters_in(k):
        for j in range(1, tp_size):
            ref = outs.at[both(chip(-sgn * k)), quarter(tp - j)]
            pltpu.make_async_remote_copy(
                src_ref=ref, dst_ref=ref, send_sem=spread_send, recv_sem=spread_recv.at[j - 1, k],
                device_id={"tp": lax.rem(tp + j, tp_size)}, device_id_type=MESH,
            ).wait_recv()
            cross(3, ref).start()

    def halo_copy():
        return pltpu.make_async_remote_copy(
            src_ref=tokens.at[pl.ds(rows - HALO, HALO)], dst_ref=tok.at[pl.ds(0, HALO)],
            send_sem=halo_send, recv_sem=halo_recv, device_id=follower, device_id_type=MESH,
        )

    for copy in loads[:3]:
        copy.wait()
    pl.semaphore_wait(barrier, len(peers))
    reach_here = jnp.where(core == 1, reaches[1], reaches[0])
    launch(0, mine, 0, core, reach_here)
    to_partner(0).start()
    for copy in loads[3:]:
        copy.wait()
    for s in (2, 1):
        launch(s, mine, 0, core, reach_here)
        to_partner(s).start()
    for s in (0, 2, 1):
        from_partner(s).wait_recv()
        launch(s, one(z, 1 - core), 0, 1 - core, reach_here)

    @pl.when(sp < 2 * chips - 1)
    def _():
        halo_copy().start()

    @pl.when(sp == 0)
    def _():
        tok[pl.ds(0, HALO), :] = jnp.zeros((HALO, width), BF16)

    load_tok.wait()
    blocks = total // BLOCK

    def norm_block(b):
        at = pl.ds(pl.multiple_of(lax.rem(b + 1, blocks) * BLOCK, BLOCK), BLOCK)
        x = tok[at, :].astype(F32)
        scale = lax.rsqrt(jnp.sum(x * x, axis=-1, keepdims=True) / width + EPS)
        normed[at, :] = (x * scale * pre_gain[pl.ds(0, 1), :]).astype(BF16)

    def norm_some(k, count):
        for j in range(count):
            b = (k - 1) * count + j

            @pl.when((b == blocks - 1) & (sp > 0))
            def _():
                halo_copy().wait_recv()

            @pl.when(b < blocks)
            def _():
                norm_block(b)

    for cc in range(2):

        @pl.when(core == cc)
        def _(reach=reaches[cc]):
            def step(k, carry):
                for s in (0, 2, 1):
                    relay(s, k, core, reach)
                    relay(s, k, 1 - core, reach)
                    if s == 2:
                        for j in range(1, tp_size):
                            quarter_to(k, j).start()
                norm_some(k, -(-blocks // reach))

                @pl.when(k > LAG)
                def _():
                    quarters_in(k - LAG)

                return carry

            lax.fori_loop(1, reach + 1, step, 0)

    def covering(i, reach):
        held = pl.ds(0, reach * 2 * depth)
        if i < 2:
            return buffers[i].at[held]
        return outs.at[held, pl.ds(0, 2 * chans * (1 if i == 2 else tp_size - 1))]

    def arrived(i):
        for cc in range(2):

            @pl.when(core == cc)
            def _():
                cross(i, covering(i, reaches[1 - cc])).wait_recv()

    def mixing(layer):
        product = jnp.dot(normed[...], gates[layer][...], preferred_element_type=F32)
        outer = product[:, :chans].astype(BF16).astype(F32)
        inner = product[:, chans : 2 * chans].astype(BF16).astype(F32)
        values = product[:, 2 * chans :].astype(BF16).astype(F32)
        gated = (inner * values).astype(BF16).astype(F32)
        here = pl.ds(pl.multiple_of(tp * chans, chans), chans)
        taps = conv_taps[:, layer, here]
        filtered = (
            taps[0:1, :] * pltpu.roll(gated, 2, axis=0)
            + taps[1:2, :] * pltpu.roll(gated, 1, axis=0)
            + taps[2:3, :] * gated
        )
        return (outer * filtered).astype(BF16)

    def mix_norm(raw, layer):
        x = raw.astype(F32)
        scale = lax.rsqrt(jnp.sum(x * x, axis=-1, keepdims=True) / channels + EPS)
        return (x * scale * mix_gain[pl.ds(layer, 1), :]).astype(BF16)

    def lanes(j):
        return pl.ds(pl.multiple_of(lax.rem(j + tp_size, tp_size) * chans, chans), chans)

    arrived(0)
    mixed_all[:, lanes(tp)] = mixing(0)
    half = (total // BLOCK + 1) // 2 * BLOCK
    parts = (pl.ds(0, half), pl.ds(half, total - half))

    def swap(i, part, owner, to):
        ref = mixed_all.at[parts[part], lanes(owner)]
        return pltpu.make_async_remote_copy(
            src_ref=ref, dst_ref=ref, send_sem=x_send.at[i], recv_sem=x_recv.at[i], device_id=to, device_id_type=MESH
        )

    swap(0, 0, tp, right).start()
    swap(2, 1, tp, left).start()
    swap(1, 1, tp, right).start()
    swap(3, 0, tp, left).start()
    swap(0, 0, tp - 1, right).wait_recv()
    swap(4, 0, tp - 1, right).start()
    swap(2, 1, tp + 1, left).wait_recv()
    swap(5, 1, tp + 1, left).start()

    for lag in reversed(range(LAG)):
        quarters_in(reach_here - lag)
    arrived(2)
    arrived(3)
    swap(1, 1, tp - 1, right).wait_recv()
    swap(3, 0, tp + 1, left).wait_recv()
    swap(4, 0, tp + 2, right).wait_recv()
    swap(5, 1, tp + 2, left).wait_recv()
    mixed_norm[...] = mix_norm(mixed_all[...], 0)
    tile = 2 * LANES
    tiles = width // tile

    def weights(cols, layer):
        return jnp.concatenate(
            [outs[cols, pl.ds((2 * j + layer) * chans, chans)] for j in range(tp_size)], axis=1
        )

    def fold(x):
        return x[:, :LANES] + x[:, LANES:]

    squares[...] = jnp.zeros_like(squares)

    def project(n, carry):
        cols = pl.ds(pl.multiple_of(n * tile, tile), tile)
        out = lax.dot_general(
            mixed_norm[...], weights(cols, 0), (((1,), (1,)), ((), ())), preferred_element_type=F32
        ).astype(BF16)
        branch[:, cols] = out
        wide = out.astype(F32)
        squares[...] += fold(wide * wide)
        return carry

    lax.fori_loop(0, tiles, project, 0)
    group = max(g for g in (4, 3, 2, 1) if blocks % g == 0) * BLOCK
    strips = width // LANES

    def row_scale(sums):
        return jnp.broadcast_to(lax.rsqrt(jnp.sum(sums, axis=-1, keepdims=True) / width + EPS), sums.shape)

    squares[...] = row_scale(squares[...])

    def next_stream(i, carry):
        at = pl.ds(pl.multiple_of(i * group, BLOCK), group)
        scale = squares[at, :]
        sums = jnp.zeros((group, LANES), F32)
        for n in range(strips):
            cols = pl.ds(n * LANES, LANES)
            new = tok[at, cols].astype(F32) + branch[at, cols].astype(F32) * scale * post_gain[pl.ds(0, 1), cols]
            stream[at, cols] = new
            sums = sums + new * new
        squares[at, :] = sums
        return carry

    lax.fori_loop(0, total // group, next_stream, 0)
    squares[...] = row_scale(squares[...])

    def next_normed(i, carry):
        at = pl.ds(pl.multiple_of(i * group, BLOCK), group)
        scale = squares[at, :]
        for n in range(strips):
            cols = pl.ds(n * LANES, LANES)
            normed[at, cols] = (stream[at, cols] * scale * pre_gain[pl.ds(1, 1), cols]).astype(BF16)
        return carry

    lax.fori_loop(0, total // group, next_normed, 0)
    arrived(1)

    mixed_own[...] = mixing(1)[HALO:, :]

    def spread(j):
        to = lax.rem(tp + j, tp_size)
        return pltpu.make_async_remote_copy(
            src_ref=mixed_own.at[pl.ds(pl.multiple_of(to * share, share), share)],
            dst_ref=mixed_rows.at[:, lanes(tp)],
            send_sem=a_send.at[j], recv_sem=a_recv.at[j], device_id={"tp": to}, device_id_type=MESH,
        )

    def gathered(j):
        ref = mixed_rows.at[:, lanes(tp - j)]
        return pltpu.make_async_remote_copy(
            src_ref=ref, dst_ref=ref, send_sem=a_send.at[j], recv_sem=a_recv.at[j],
            device_id={"tp": lax.rem(tp + j, tp_size)}, device_id_type=MESH,
        )

    order = [2, 1, 3] if tp_size == 4 else list(range(1, tp_size))
    for j in order:
        spread(j).start()
    own_rows = pl.ds(pl.multiple_of(tp * share, share), share)
    mixed_rows[:, lanes(tp)] = mixed_own[own_rows, :]
    for j in order:
        gathered(j).wait_recv()
    mixed = mix_norm(mixed_rows[...], 1)
    sums = jnp.zeros((share, LANES), F32)
    for n in range(tiles):
        cols = pl.ds(n * tile, tile)
        out = lax.dot_general(
            mixed, weights(cols, 1), (((1,), (1,)), ((), ())), preferred_element_type=F32
        ).astype(BF16)
        branch[pl.ds(0, share), cols] = out
        wide = out.astype(F32)
        sums = sums + fold(wide * wide)
    scale = row_scale(sums)
    held = pl.ds(pl.multiple_of(HALO + tp * share, BLOCK), share)
    for n in range(strips):
        cols = pl.ds(n * LANES, LANES)
        new = stream[held, cols] + branch[pl.ds(0, share), cols].astype(F32) * scale * post_gain[pl.ds(1, 1), cols]
        result[:, cols] = new.astype(BF16)

    @pl.when(sp < 2 * chips - 1)
    def _():
        halo_copy().wait_send()

    for j in order:
        spread(j).wait_send()
    for i, part in ((0, 0), (1, 1), (2, 1), (3, 0), (4, 0), (5, 1)):
        swap(i, part, tp, right).wait_send()
    for s in range(3):
        to_partner(s).wait_send()
    for cc in range(2):

        @pl.when(core == cc)
        def _(reach=reaches[cc]):
            for i in range(4):
                cross(i, covering(i, reach)).wait_send()
            for i in range(3):
                along_all = pltpu.make_async_remote_copy(
                    src_ref=covering(i, reach), dst_ref=covering(i, reach), send_sem=ring_send.at[i],
                    recv_sem=ring_recv.at[0, 0, 0], device_id=ahead, device_id_type=MESH,
                )
                along_all.wait_send()
            pltpu.make_async_remote_copy(
                src_ref=covering(3, reach), dst_ref=covering(3, reach), send_sem=spread_send,
                recv_sem=ring_recv.at[0, 0, 0], device_id=right, device_id_type=MESH,
            ).wait_send()


def solution(mesh):
    chips = mesh.shape["sp"] // 2
    tp_size = mesh.shape["tp"]

    def per_device(tokens, gate_in, gate_conv, value_in, out_weight, conv_taps, pre_gain, mix_gain, post_gain):
        rows, width = tokens.shape
        depth, chans = gate_in.shape[1:]
        channels = tp_size * chans
        total = rows + HALO
        share = rows // tp_size
        sizes = (chips, tp_size, depth, rows, width, chans)
        anywhere = pl.BlockSpec(memory_space=pl.ANY)
        inside = pl.BlockSpec(memory_space=pltpu.VMEM)
        dma = pltpu.SemaphoreType.DMA
        return pl.pallas_call(
            functools.partial(block_kernel, sizes),
            out_shape=jax.ShapeDtypeStruct((share, width), BF16),
            in_specs=[anywhere] * 5 + [inside] * 4,
            out_specs=inside,
            scratch_shapes=[
                pltpu.VMEM((width, 3 * chans), BF16),
                pltpu.VMEM((width, 3 * chans), BF16),
                pltpu.VMEM((width, 2 * channels), BF16),
                pltpu.VMEM((total, width), BF16),
                pltpu.VMEM((total, width), BF16),
                pltpu.VMEM((total, width), BF16),
                pltpu.VMEM((total, width), F32),
                pltpu.VMEM((total, channels), BF16),
                pltpu.VMEM((total, channels), BF16),
                pltpu.VMEM((rows, chans), BF16),
                pltpu.VMEM((share, channels), BF16),
                pltpu.VMEM((total, LANES), F32),
                dma((7 + 2 * tp_size,)),
                dma((4,)),
                dma((4,)),
                dma((4,)),
                dma((4,)),
                dma((4,)),
                dma((3, 2, chips)),
                dma,
                dma,
                dma((6,)),
                dma((6,)),
                dma,
                dma((tp_size - 1, chips)),
                dma((tp_size,)),
                dma((tp_size,)),
            ],
            compiler_params=pltpu.CompilerParams(
                collective_id=0, has_side_effects=True, vmem_limit_bytes=56 * 2**20
            ),
            name="blocks",
        )(
            tokens,
            gate_in,
            gate_conv,
            value_in,
            jnp.swapaxes(out_weight, 1, 2),
            jnp.swapaxes(conv_taps, 0, 1),
            pre_gain,
            mix_gain,
            post_gain,
        )

    return jax.shard_map(
        per_device,
        mesh=mesh,
        in_specs=(
            P(("grp", "sp"), None),
            P(None, "sp", "tp"),
            P(None, "sp", "tp"),
            P(None, "sp", "tp"),
            P(None, None, "sp"),
            P(),
            P(),
            P(),
            P(),
        ),
        out_specs=P(("grp", "sp", "tp"), None),
        check_vma=False,
    )
```

```python
import functools

import jax
import jax.numpy as jnp
from jax import lax
from jax.experimental import pallas as pl
from jax.experimental.pallas import tpu as pltpu
from jax.sharding import PartitionSpec as P

EPS = 1e-06
MESH = pl.DeviceIdType.MESH
F32 = jnp.float32
BF16 = jnp.bfloat16
LANES = 128
HALO = 16
BLOCK = 16
LAG = 2


def block_kernel(
    sizes,
    tokens,
    gate_in,
    gate_conv,
    value_in,
    out_weight,
    conv_taps,
    pre_gain,
    mix_gain,
    post_gain,
    result,
    gates0,
    gates1,
    outs,
    tok,
    normed,
    branch,
    stream,
    mixed_all,
    mixed_norm,
    mixed_own,
    mixed_rows,
    squares,
    load_sem,
    inj_send,
    inj_recv,
    cross_send,
    cross_recv,
    ring_send,
    ring_recv,
    halo_send,
    halo_recv,
    x_send,
    x_recv,
    spread_send,
    spread_recv,
    a_send,
    a_recv,
):
    chips, tp_size, depth, rows, width, chans = sizes
    channels = tp_size * chans
    total = rows + HALO
    share = rows // tp_size
    sp = lax.axis_index("sp")
    tp = lax.axis_index("tp")
    z = sp // 2
    core = lax.rem(sp, 2)
    sgn = 1 - 2 * core
    minus = (9 * chips) // 16
    reaches = (chips - 1 - minus, minus)

    def chip(k):
        return lax.rem(z + k + 2 * chips, chips)

    partner = {"sp": z * 2 + 1 - core}
    ahead = {"sp": chip(sgn) * 2 + core}
    behind = {"sp": chip(-sgn) * 2 + core}
    follower = {"sp": lax.rem(sp + 1, 2 * chips)}
    leader = {"sp": lax.rem(sp + 2 * chips - 1, 2 * chips)}
    across = {"sp": jnp.where(core == 1, lax.rem(sp + 1, 2 * chips), lax.rem(sp + 2 * chips - 1, 2 * chips))}
    right = {"tp": lax.rem(tp + 1, tp_size)}
    left = {"tp": lax.rem(tp + tp_size - 1, tp_size)}

    barrier = pltpu.get_barrier_semaphore()
    peers = [partner, ahead, behind, across]
    peers += [{"tp": lax.rem(tp + j, tp_size)} for j in range(1, tp_size)]
    for peer in peers:
        pl.semaphore_signal(barrier, inc=1, device_id=peer, device_id_type=MESH)

    mine = pl.ds(pl.multiple_of(sp * depth, depth), depth)
    gates = (gates0, gates1)
    loads = []
    for layer in range(2):
        for j, weight in enumerate((gate_in, gate_conv, value_in)):
            copy = pltpu.make_async_copy(
                weight.at[layer], gates[layer].at[mine, pl.ds(j * chans, chans)], load_sem.at[3 * layer + j]
            )
            copy.start()
            loads.append(copy)
    for layer in range(2):
        for j in range(tp_size):
            copy = pltpu.make_async_copy(
                out_weight.at[layer, :, pl.ds(j * chans, chans)],
                outs.at[mine, pl.ds((2 * j + layer) * chans, chans)],
                load_sem.at[7 + layer * tp_size + j],
            )
            copy.start()
            loads.append(copy)
    load_tok = pltpu.make_async_copy(tokens, tok.at[pl.ds(HALO, rows)], load_sem.at[6])
    load_tok.start()

    buffers = (gates0, gates1, outs)

    def quarter(j):
        return pl.ds(pl.multiple_of(lax.rem(j + tp_size, tp_size) * 2 * chans, 2 * chans), 2 * chans)

    def part(s, block):
        return outs.at[block, quarter(tp)] if s == 2 else buffers[s].at[block]

    def one(zz, cc):
        return pl.ds(pl.multiple_of((zz * 2 + cc) * depth, depth), depth)

    def both(zz):
        return pl.ds(pl.multiple_of(zz * 2 * depth, 2 * depth), 2 * depth)

    def to_partner(s):
        ref = buffers[s].at[mine]
        return pltpu.make_async_remote_copy(
            src_ref=ref, dst_ref=ref, send_sem=inj_send.at[s], recv_sem=inj_recv.at[s],
            device_id=partner, device_id_type=MESH,
        )

    def from_partner(s):
        ref = buffers[s].at[one(z, 1 - core)]
        return pltpu.make_async_remote_copy(
            src_ref=ref, dst_ref=ref, send_sem=inj_send.at[s], recv_sem=inj_recv.at[s],
            device_id=partner, device_id_type=MESH,
        )

    def along(s, block, sem, to):
        ref = part(s, block)
        return pltpu.make_async_remote_copy(
            src_ref=ref, dst_ref=ref, send_sem=ring_send.at[s], recv_sem=sem, device_id=to, device_id_type=MESH
        )

    def cross(i, ref):
        return pltpu.make_async_remote_copy(
            src_ref=ref, dst_ref=ref, send_sem=cross_send.at[i], recv_sem=cross_recv.at[i],
            device_id=partner, device_id_type=MESH,
        )

    def launch(s, block, k, sub, reach):
        @pl.when(k < reach)
        def _():
            along(s, block, ring_recv.at[s, sub, k + 1], ahead).start()

    def relay(s, k, sub, reach):
        block = one(chip(-sgn * k), sub)
        along(s, block, ring_recv.at[s, sub, k], ahead).wait_recv()
        launch(s, block, k, sub, reach)
        cross(s, part(s, block)).start()

    def quarter_to(k, j):
        ref = outs.at[both(chip(-sgn * k)), quarter(tp)]
        return pltpu.make_async_remote_copy(
            src_ref=ref, dst_ref=ref, send_sem=spread_send, recv_sem=spread_recv.at[j - 1, k],
            device_id={"tp": lax.rem(tp + j, tp_size)}, device_id_type=MESH,
        )

    def quarters_in(k):
        for j in range(1, tp_size):
            ref = outs.at[both(chip(-sgn * k)), quarter(tp - j)]
            pltpu.make_async_remote_copy(
                src_ref=ref, dst_ref=ref, send_sem=spread_send, recv_sem=spread_recv.at[j - 1, k],
                device_id={"tp": lax.rem(tp + j, tp_size)}, device_id_type=MESH,
            ).wait_recv()
            cross(3, ref).start()

    def halo_copy():
        return pltpu.make_async_remote_copy(
            src_ref=tokens.at[pl.ds(rows - HALO, HALO)], dst_ref=tok.at[pl.ds(0, HALO)],
            send_sem=halo_send, recv_sem=halo_recv, device_id=follower, device_id_type=MESH,
        )

    for copy in loads[:3]:
        copy.wait()
    pl.semaphore_wait(barrier, len(peers))
    reach_here = jnp.where(core == 1, reaches[1], reaches[0])
    launch(0, mine, 0, core, reach_here)
    to_partner(0).start()
    for copy in loads[3:]:
        copy.wait()
    for s in (2, 1):
        launch(s, mine, 0, core, reach_here)
        to_partner(s).start()
    for s in (0, 2, 1):
        from_partner(s).wait_recv()
        launch(s, one(z, 1 - core), 0, 1 - core, reach_here)

    @pl.when(sp < 2 * chips - 1)
    def _():
        halo_copy().start()

    @pl.when(sp == 0)
    def _():
        tok[pl.ds(0, HALO), :] = jnp.zeros((HALO, width), BF16)

    load_tok.wait()
    blocks = total // BLOCK

    def norm_block(b):
        at = pl.ds(pl.multiple_of(lax.rem(b + 1, blocks) * BLOCK, BLOCK), BLOCK)
        x = tok[at, :].astype(F32)
        scale = lax.rsqrt(jnp.sum(x * x, axis=-1, keepdims=True) / width + EPS)
        normed[at, :] = (x * scale * pre_gain[pl.ds(0, 1), :]).astype(BF16)

    def norm_some(k, count):
        for j in range(count):
            b = (k - 1) * count + j

            @pl.when((b == blocks - 1) & (sp > 0))
            def _():
                halo_copy().wait_recv()

            @pl.when(b < blocks)
            def _():
                norm_block(b)

    for cc in range(2):

        @pl.when(core == cc)
        def _(reach=reaches[cc]):
            def step(k, carry):
                for s in (0, 2, 1):
                    relay(s, k, core, reach)
                    relay(s, k, 1 - core, reach)
                    if s == 2:
                        for j in range(1, tp_size):
                            quarter_to(k, j).start()
                norm_some(k, -(-blocks // reach))

                @pl.when(k > LAG)
                def _():
                    quarters_in(k - LAG)

                return carry

            lax.fori_loop(1, reach + 1, step, 0)

    def covering(i, reach):
        held = pl.ds(0, reach * 2 * depth)
        if i < 2:
            return buffers[i].at[held]
        return outs.at[held, pl.ds(0, 2 * chans * (1 if i == 2 else tp_size - 1))]

    def arrived(i):
        for cc in range(2):

            @pl.when(core == cc)
            def _():
                cross(i, covering(i, reaches[1 - cc])).wait_recv()

    def mixing(layer):
        product = jnp.dot(normed[...], gates[layer][...], preferred_element_type=F32)
        outer = product[:, :chans].astype(BF16).astype(F32)
        inner = product[:, chans : 2 * chans].astype(BF16).astype(F32)
        values = product[:, 2 * chans :].astype(BF16).astype(F32)
        gated = (inner * values).astype(BF16).astype(F32)
        here = pl.ds(pl.multiple_of(tp * chans, chans), chans)
        taps = conv_taps[:, layer, here]
        filtered = (
            taps[0:1, :] * pltpu.roll(gated, 2, axis=0)
            + taps[1:2, :] * pltpu.roll(gated, 1, axis=0)
            + taps[2:3, :] * gated
        )
        return (outer * filtered).astype(BF16)

    def mix_norm(raw, layer):
        x = raw.astype(F32)
        scale = lax.rsqrt(jnp.sum(x * x, axis=-1, keepdims=True) / channels + EPS)
        return (x * scale * mix_gain[pl.ds(layer, 1), :]).astype(BF16)

    def lanes(j):
        return pl.ds(pl.multiple_of(lax.rem(j + tp_size, tp_size) * chans, chans), chans)

    arrived(0)
    mixed_all[:, lanes(tp)] = mixing(0)

    def swap(j, owner):
        ref = mixed_all.at[:, lanes(owner)]
        return pltpu.make_async_remote_copy(
            src_ref=ref, dst_ref=ref, send_sem=x_send.at[j], recv_sem=x_recv.at[j],
            device_id={"tp": lax.rem(tp + j, tp_size)}, device_id_type=MESH,
        )

    order = [2, 1, 3] if tp_size == 4 else list(range(1, tp_size))
    for j in order:
        swap(j, tp).start()

    for lag in reversed(range(LAG)):
        quarters_in(reach_here - lag)
    arrived(2)
    arrived(3)
    for j in order:
        swap(j, tp - j).wait_recv()
    mixed_norm[...] = mix_norm(mixed_all[...], 0)
    tile = 2 * LANES
    tiles = width // tile

    def weights(cols, layer):
        return jnp.concatenate(
            [outs[cols, pl.ds((2 * j + layer) * chans, chans)] for j in range(tp_size)], axis=1
        )

    def fold(x):
        return x[:, :LANES] + x[:, LANES:]

    squares[...] = jnp.zeros_like(squares)

    def project(n, carry):
        cols = pl.ds(pl.multiple_of(n * tile, tile), tile)
        out = lax.dot_general(
            mixed_norm[...], weights(cols, 0), (((1,), (1,)), ((), ())), preferred_element_type=F32
        ).astype(BF16)
        branch[:, cols] = out
        wide = out.astype(F32)
        squares[...] += fold(wide * wide)
        return carry

    lax.fori_loop(0, tiles, project, 0)
    group = max(g for g in (4, 3, 2, 1) if blocks % g == 0) * BLOCK
    strips = width // LANES

    def row_scale(sums):
        return jnp.broadcast_to(lax.rsqrt(jnp.sum(sums, axis=-1, keepdims=True) / width + EPS), sums.shape)

    squares[...] = row_scale(squares[...])

    def next_stream(i, carry):
        at = pl.ds(pl.multiple_of(i * group, BLOCK), group)
        scale = squares[at, :]
        sums = jnp.zeros((group, LANES), F32)
        for n in range(strips):
            cols = pl.ds(n * LANES, LANES)
            new = tok[at, cols].astype(F32) + branch[at, cols].astype(F32) * scale * post_gain[pl.ds(0, 1), cols]
            stream[at, cols] = new
            sums = sums + new * new
        squares[at, :] = sums
        return carry

    lax.fori_loop(0, total // group, next_stream, 0)
    squares[...] = row_scale(squares[...])

    def next_normed(i, carry):
        at = pl.ds(pl.multiple_of(i * group, BLOCK), group)
        scale = squares[at, :]
        for n in range(strips):
            cols = pl.ds(n * LANES, LANES)
            normed[at, cols] = (stream[at, cols] * scale * pre_gain[pl.ds(1, 1), cols]).astype(BF16)
        return carry

    lax.fori_loop(0, total // group, next_normed, 0)
    arrived(1)

    mixed_own[...] = mixing(1)[HALO:, :]

    def spread(j):
        to = lax.rem(tp + j, tp_size)
        return pltpu.make_async_remote_copy(
            src_ref=mixed_own.at[pl.ds(pl.multiple_of(to * share, share), share)],
            dst_ref=mixed_rows.at[:, lanes(tp)],
            send_sem=a_send.at[j], recv_sem=a_recv.at[j], device_id={"tp": to}, device_id_type=MESH,
        )

    def gathered(j):
        ref = mixed_rows.at[:, lanes(tp - j)]
        return pltpu.make_async_remote_copy(
            src_ref=ref, dst_ref=ref, send_sem=a_send.at[j], recv_sem=a_recv.at[j],
            device_id={"tp": lax.rem(tp + j, tp_size)}, device_id_type=MESH,
        )

    order = [2, 1, 3] if tp_size == 4 else list(range(1, tp_size))
    for j in order:
        spread(j).start()
    own_rows = pl.ds(pl.multiple_of(tp * share, share), share)
    mixed_rows[:, lanes(tp)] = mixed_own[own_rows, :]
    for j in order:
        gathered(j).wait_recv()
    mixed = mix_norm(mixed_rows[...], 1)
    sums = jnp.zeros((share, LANES), F32)
    for n in range(tiles):
        cols = pl.ds(n * tile, tile)
        out = lax.dot_general(
            mixed, weights(cols, 1), (((1,), (1,)), ((), ())), preferred_element_type=F32
        ).astype(BF16)
        branch[pl.ds(0, share), cols] = out
        wide = out.astype(F32)
        sums = sums + fold(wide * wide)
    scale = row_scale(sums)
    held = pl.ds(pl.multiple_of(HALO + tp * share, BLOCK), share)
    for n in range(strips):
        cols = pl.ds(n * LANES, LANES)
        new = stream[held, cols] + branch[pl.ds(0, share), cols].astype(F32) * scale * post_gain[pl.ds(1, 1), cols]
        result[:, cols] = new.astype(BF16)

    @pl.when(sp < 2 * chips - 1)
    def _():
        halo_copy().wait_send()

    for j in order:
        spread(j).wait_send()
    for j in order:
        swap(j, tp).wait_send()
    for s in range(3):
        to_partner(s).wait_send()
    for cc in range(2):

        @pl.when(core == cc)
        def _(reach=reaches[cc]):
            for i in range(4):
                cross(i, covering(i, reach)).wait_send()
            for i in range(3):
                along_all = pltpu.make_async_remote_copy(
                    src_ref=covering(i, reach), dst_ref=covering(i, reach), send_sem=ring_send.at[i],
                    recv_sem=ring_recv.at[0, 0, 0], device_id=ahead, device_id_type=MESH,
                )
                along_all.wait_send()
            pltpu.make_async_remote_copy(
                src_ref=covering(3, reach), dst_ref=covering(3, reach), send_sem=spread_send,
                recv_sem=ring_recv.at[0, 0, 0], device_id=right, device_id_type=MESH,
            ).wait_send()


def solution(mesh):
    chips = mesh.shape["sp"] // 2
    tp_size = mesh.shape["tp"]

    def per_device(tokens, gate_in, gate_conv, value_in, out_weight, conv_taps, pre_gain, mix_gain, post_gain):
        rows, width = tokens.shape
        depth, chans = gate_in.shape[1:]
        channels = tp_size * chans
        total = rows + HALO
        share = rows // tp_size
        sizes = (chips, tp_size, depth, rows, width, chans)
        anywhere = pl.BlockSpec(memory_space=pl.ANY)
        inside = pl.BlockSpec(memory_space=pltpu.VMEM)
        dma = pltpu.SemaphoreType.DMA
        return pl.pallas_call(
            functools.partial(block_kernel, sizes),
            out_shape=jax.ShapeDtypeStruct((share, width), BF16),
            in_specs=[anywhere] * 5 + [inside] * 4,
            out_specs=inside,
            scratch_shapes=[
                pltpu.VMEM((width, 3 * chans), BF16),
                pltpu.VMEM((width, 3 * chans), BF16),
                pltpu.VMEM((width, 2 * channels), BF16),
                pltpu.VMEM((total, width), BF16),
                pltpu.VMEM((total, width), BF16),
                pltpu.VMEM((total, width), BF16),
                pltpu.VMEM((total, width), F32),
                pltpu.VMEM((total, channels), BF16),
                pltpu.VMEM((total, channels), BF16),
                pltpu.VMEM((rows, chans), BF16),
                pltpu.VMEM((share, channels), BF16),
                pltpu.VMEM((total, LANES), F32),
                dma((7 + 2 * tp_size,)),
                dma((4,)),
                dma((4,)),
                dma((4,)),
                dma((4,)),
                dma((4,)),
                dma((3, 2, chips)),
                dma,
                dma,
                dma((6,)),
                dma((6,)),
                dma,
                dma((tp_size - 1, chips)),
                dma((tp_size,)),
                dma((tp_size,)),
            ],
            compiler_params=pltpu.CompilerParams(
                collective_id=0, has_side_effects=True, vmem_limit_bytes=56 * 2**20
            ),
            name="blocks",
        )(
            tokens,
            gate_in,
            gate_conv,
            value_in,
            jnp.swapaxes(out_weight, 1, 2),
            jnp.swapaxes(conv_taps, 0, 1),
            pre_gain,
            mix_gain,
            post_gain,
        )

    return jax.shard_map(
        per_device,
        mesh=mesh,
        in_specs=(
            P(("grp", "sp"), None),
            P(None, "sp", "tp"),
            P(None, "sp", "tp"),
            P(None, "sp", "tp"),
            P(None, None, "sp"),
            P(),
            P(),
            P(),
            P(),
        ),
        out_specs=P(("grp", "sp", "tp"), None),
        check_vma=False,
    )
```
